32 devices in a mesh: fs: 16 (over z, y, x), tp: 2 (over core).
Axes of the slice: x: 2, y: 2, z: 4, core: 2. Of those that a mesh axis runs over, the one named last changes fastest.
Arguments:
- fwd_input: bfloat16 [2048, 2048], P('fs'), may hold values from -6 to 6
- saved_input: bfloat16 [2048, 2048], P('fs'), may hold values from -6 to 6
- out_cotangent: bfloat16 [2048, 2048], P('fs'), may hold values from -6 to 6
- up_weight: bfloat16 [2048, 4096], P('fs', 'tp'), may hold values from -0.125 to 0.125
- down_weight: bfloat16 [4096, 2048], P('tp', 'fs'), may hold values from -0.09375 to 0.09375
- up_grad_sum: float32 [2048, 4096], P('fs', 'tp'), may hold values from -6 to 6
Outputs:
- layer_out: bfloat16 [2048, 2048], P('fs')
- input_grad: bfloat16 [2048, 2048], P('fs')
- up_grad_out: float32 [2048, 4096], P('fs', 'tp')
The draws below stay inside these ranges and needn't reach their ends.
All inputs are finite; a program needn't handle non-finite values.
Results may differ from the reference program's by a relative error of at most 0.013.
Values may be sent and summed in bfloat16 or wider, within the bound.
A program may use at most 128 MiB of HBM per device.

```python
import jax
import jax.numpy as jnp
from jax import lax

D = 2048
FF = 4096
TOKENS = 2048
N_TP = 2


def spiked(entries, key, source, target, parts, factor):
    owner, partner = [(jnp.arange(entries.shape[axis_at]) // (entries.shape[axis_at] // parts)).reshape([-1 if axis == axis_at else 1 for axis in range(entries.ndim)]) for axis_at in (source, target)]
    chosen = jax.random.permutation(key, parts)[partner]
    strong = (owner == chosen) | (owner == (partner + parts // 2) % parts)
    return jnp.where(strong, factor * entries, entries)


def level_of(own_key, dims, cuts, least, top_value):
    loudness, own = 1.0, jax.random.fold_in(own_key, 6)
    for position, shards_of in cuts:
        steps = jnp.exp(jax.random.uniform(jax.random.fold_in(own, position), (shards_of,), jnp.float32, least / len(cuts), top_value / len(cuts)))
        loudness = loudness * jnp.repeat(steps, dims[position] // shards_of).reshape([-1 if axis == position else 1 for axis in range(len(dims))])
    return loudness


def centred(stream_key, dims, spread, limit, cuts=(), held_as=jnp.bfloat16):
    loudness = level_of(stream_key, dims, cuts, -0.22, 0.18) if cuts else 1.0
    drawn = jax.random.normal(stream_key, dims, jnp.float32) * spread * loudness
    return jnp.minimum(jnp.maximum(drawn, -limit), limit).astype(held_as)


def bell_draw_with(key, shape, scale, most, pieces, heavy, dtype=jnp.bfloat16):
    values = scale * jax.random.normal(key, shape, jnp.float32)
    if pieces:
        values = values * level_of(key, shape, pieces, -0.22, 0.18)
    return jnp.clip(spiked(values, jax.random.fold_in(key, 3), *heavy), -most, most).astype(dtype)


def setup_inputs(seed: int = 0) -> dict:
    splits = jax.random.split(jax.random.key(seed), 7)
    fwd_input = centred(splits[0], (TOKENS, D), 1.0, 6.0, ((0, 16),))
    saved_input = bell_draw_with(splits[1], (TOKENS, D), 1.0, 6.0, ((0, 16),), (0, 1, 16, 2.0))
    out_cotangent = bell_draw_with(splits[2], (TOKENS, D), 1.0, 6.0, ((0, 16),), (0, 1, 16, 2.0))
    up_weight = centred(splits[3], (D, FF), D ** -0.5, 0.125, ((0, 16), (1, 2)))
    down_weight = centred(splits[4], (FF, D), FF ** -0.5, 0.09375, ((0, 2), (1, 16)))
    up_grad_sum = centred(splits[5], (D, FF), 1.0, 6.0, ((0, 16), (1, 2)), jnp.float32)
    return {"fwd_input": fwd_input, "saved_input": saved_input, "out_cotangent": out_cotangent, "up_weight": up_weight, "down_weight": down_weight, "up_grad_sum": up_grad_sum}


def split_sum(left, right):
    block = right.shape[0] // N_TP
    running = jnp.zeros((left.shape[0], right.shape[1]), jnp.float32)
    for index in range(N_TP):
        partial_out = jnp.dot(left[:, index * block:(index + 1) * block], right[index * block:(index + 1) * block], preferred_element_type=jnp.float32)
        rounded = lax.optimization_barrier(partial_out.astype(jnp.bfloat16))
        running = running + rounded.astype(jnp.float32)
    return running.astype(jnp.bfloat16)


def reference(fwd_input, saved_input, out_cotangent, up_weight, down_weight, up_grad_sum):
    pre_fwd = jnp.dot(fwd_input, up_weight, preferred_element_type=jnp.float32)
    positive = jnp.maximum(pre_fwd, 0.0)
    hidden = (positive * positive).astype(jnp.bfloat16)
    layer_out = split_sum(hidden, down_weight)
    pre_bwd = jnp.dot(saved_input, up_weight, preferred_element_type=jnp.float32)
    d_hidden = jnp.dot(out_cotangent, down_weight.T, preferred_element_type=jnp.float32)
    d_pre = (d_hidden * 2.0 * jnp.maximum(pre_bwd, 0.0)).astype(jnp.bfloat16)
    input_grad = split_sum(d_pre, up_weight.T)
    up_grad = jnp.dot(saved_input.T, d_pre, preferred_element_type=jnp.float32)
    up_grad_out = up_grad_sum + up_grad * (float(TOKENS) ** -0.5)
    return layer_out, input_grad, up_grad_out
```

```python
import functools

import jax
import jax.numpy as jnp
from jax import lax
from jax.experimental import pallas as pl
from jax.experimental.pallas import tpu as pltpu
from jax.sharding import PartitionSpec as P

MESH = pl.DeviceIdType.MESH
F32 = jnp.float32
BF16 = jnp.bfloat16
PARTS = [256, 128, 128]
SCHEDULE = [('slices', 0), ('pieces', 0), ('pieces', 1), ('slices', 1), ('slices', 2), ('collect', 0, 0), ('over', 1), ('collect', 0, 1), ('relay', 0, 0, 1), ('relay', 0, 1, 1), ('near', 1), ('near', 2), ('pieces', 2), ('near', 0), ('over', 2), ('over', 0), ('take', 2, 1), ('collect', 1, 0), ('relay', 0, 0, 2), ('relay', 0, 0, 3), ('take', 1, 0), ('take', 0, 1), ('relay', 0, 1, 2), ('collect', 1, 1), ('keep_own',), ('collect', 2, 0), ('take', 1, 1), ('collect', 2, 1), ('relay', 0, 1, 3), ('relay', 1, 0, 1), ('take', 2, 0), ('take', 1, 2), ('take', 2, 2), ('settle', 1), ('settle', 2), ('take', 0, 0), ('backward', 0), ('grads', 0), ('relay', 1, 0, 2), ('relay', 2, 0, 1), ('relay', 1, 0, 3), ('relay', 1, 1, 1), ('relay', 1, 1, 2), ('take', 0, 2), ('relay', 1, 1, 3), ('settle', 0), ('backward', 1), ('grads', 1), ('forward', 0), ('forward', 1), ('relay', 2, 0, 2), ('relay', 2, 0, 3), ('forward', 2), ('relay', 2, 1, 1), ('spread_at', 0), ('spread_at', 1), ('relay', 2, 1, 2), ('tp_at', 0), ('tp_at', 1), ('spread_at', 2), ('relay', 2, 1, 3), ('backward', 2), ('tp_at', 2), ('sums', 0, 1), ('sums', 0, 2), ('spread', 1, 0), ('spread', 1, 1), ('tp_sums', 1, 0), ('grads', 2), ('spread_at', 3), ('spread', 1, 2), ('tp_at', 3), ('tp_sums', 1, 1), ('near_at', 2), ('near_at', 0), ('sums', 1, 1), ('spread', 1, 3), ('tp_sums', 1, 3), ('near_at', 1), ('tp_sums', 1, 2), ('near_sums', 1, 1), ('sums', 1, 2), ('near_at', 3), ('near_sums', 1, 2), ('near_sums', 1, 0), ('sums', 2, 1), ('sums', 0, 3), ('near_sums', 1, 3), ('sums', 1, 3), ('sums', 2, 2), ('sums', 2, 3), ('finish', 0), ('finish', 1)]


def remote(src, dst, send_sem, recv_sem, fs, tp):
    return pltpu.make_async_remote_copy(
        src_ref=src,
        dst_ref=dst,
        send_sem=send_sem,
        recv_sem=recv_sem,
        device_id=(fs, tp),
        device_id_type=MESH,
    )


def kernel(
    n, T, B, parts, fwd, saved, cot, up, down, out, ing, gout,
    X, turned, O, tp_in, S, near_in, far_in, W, H, pre, G, from_left, from_right,
    wS, wR, zS, zR, aS, aR, bS, bR, tS, tR, nS, nR, mS, mR, fS, fR,
    gS, gL, gR, hS, hR,
):
    L = n // B
    f, t = lax.axis_index("fs"), lax.axis_index("tp")
    h, p = lax.div(f, B), lax.rem(f, B)
    far = L - 1 - h
    rows, D = fwd.shape
    C = rows // T
    Rw, F = up.shape
    Fs = F // B
    Q = len(parts)
    tokens = B * rows
    deep = B * Rw
    K = D // deep
    a, b = lax.div(p, 2), lax.rem(p, 2)
    near, over, cross = 2 * a + 1 - b, 2 * (1 - a) + b, 2 * (1 - a) + 1 - b
    peers = [near, over, cross]
    mates = [lax.rem(t + i, T) for i in range(1, T)]
    has_left, has_right = h > 0, h < L - 1
    stages = [(c, pc) for c in range(Q) for pc in range(2)]

    left, right = f - B, f + B

    def dev(q):
        return h * B + q

    def chunk(index):
        return pl.ds(pl.multiple_of(index * C, C), C)

    def cols(index, c):
        return pl.ds(pl.multiple_of(index * Fs + sum(parts[:c]), 128), parts[c])

    barrier = pltpu.get_barrier_semaphore()
    for q in peers:
        pl.semaphore_signal(barrier, inc=1, device_id=(dev(q), t), device_id_type=MESH)
    for m in mates:
        pl.semaphore_signal(barrier, inc=1, device_id=(f, m), device_id_type=MESH)

    @pl.when(has_left)
    def _():
        pl.semaphore_signal(barrier, inc=1, device_id=(left, t), device_id_type=MESH)

    @pl.when(has_right)
    def _():
        pl.semaphore_signal(barrier, inc=1, device_id=(right, t), device_id_type=MESH)

    ends = lax.div(h + L - 1, L) + lax.div(far + L - 1, L)
    pl.semaphore_wait(barrier, len(peers) + T - 1 + ends)

    weights = (up, down if down.shape == up.shape else turned)

    def slice_out(c, pc, i, q):
        return remote(
            weights[pc].at[:, cols(q, c)], W[c].at[pc, h, p],
            wS.at[c, pc, i], wR.at[c, pc, p], dev(q), t,
        )

    def slice_in(c, pc, q):
        there = W[c].at[pc, h, q]
        return remote(there, there, wS.at[c, pc, 0], wR.at[c, pc, q], dev(q), t)

    def line_piece(c, pc, q, way):
        src = weights[pc].at[:, cols(p, c)] if q is p else W[c].at[pc, h, q]
        return remote(
            src, W[c].at[pc, h, q], zS.at[way, c, pc, h], zR.at[c, pc, h], right if way == 0 else left, t
        )

    def line(c, pc, k, way):
        block = W[c].at[pc, k]
        return remote(
            block, block, zS.at[way, c, pc, k], zR.at[c, pc, k], right if way == 0 else left, t
        )

    def push(c, pc, q):
        @pl.when(has_right)
        def _():
            line_piece(c, pc, q, 0).start()

        @pl.when(has_left)
        def _():
            line_piece(c, pc, q, 1).start()

    def own_w(c, pc):
        W[c][pc, h, p] = weights[pc][:, cols(p, c)]

    def collect(c, pc):
        for q in peers:
            slice_in(c, pc, q).wait_recv()
            push(c, pc, q)

    acts = (fwd, saved, cot)

    def act_out(j, i, q):
        return remote(acts[j].at[chunk(t)], X.at[j, p, chunk(t)], aS.at[j, i], aR.at[j, p], dev(q), t)

    def act_on(j):
        q, to = (over, near) if j == 1 else (near, over)
        there = X.at[j, q, chunk(t)]
        return remote(there, there, aS.at[j, 2], aR.at[j, q], dev(to), t)

    def act_in(j, q):
        there = X.at[j, q, chunk(t)]
        return remote(there, there, aS.at[j, 0], aR.at[j, q], dev(q), t)

    def act_share(j, i, q, o, m):
        there = X.at[j, q, chunk(t)]
        return remote(there, there, bS.at[j, i, o], bR.at[j, q, t], f, m)

    def act_shared(j, i, q, o, m):
        there = X.at[j, q, chunk(m)]
        return remote(there, there, bS.at[j, i, o], bR.at[j, q, m], f, m)

    def take(j, i):
        act_in(j, peers[i]).wait_recv()
        if i == (1 if j == 1 else 0):
            act_on(j).start()
        for o, m in enumerate(mates):
            act_share(j, i, peers[i], o, m).start()

    def relay(c, pc, s):
        @pl.when(h >= s)
        def _():
            line(c, pc, h - s, 0).wait_recv()

            @pl.when(has_right)
            def _():
                line(c, pc, h - s, 0).start()

        @pl.when(far >= s)
        def _():
            line(c, pc, h + s, 1).wait_recv()

            @pl.when(has_left)
            def _():
                line(c, pc, h + s, 1).start()

    def product(c, j, pc):
        return jnp.dot(
            X[j].reshape(tokens, D), W[c][pc].reshape(D, parts[c]), preferred_element_type=F32
        )

    def forward(c):
        positive = jnp.maximum(product(c, 0, 0), 0.0)
        H[c][0] = (positive * positive).astype(BF16)

    def backward(c):
        pre[c][...] = product(c, 1, 0)
        d_hidden = product(c, 2, 1)
        H[c][1] = (d_hidden * 2.0 * jnp.maximum(pre[c][...], 0.0)).astype(BF16)

    order = []
    for i in range((L + 1) // 2):
        order += [L - 1 - i] if L - 1 - i == i else [L - 1 - i, i]

    def to_right(c, d):
        return remote(G[c].at[d], from_left[c].at[d], gS.at[c, d], gL.at[c, d], right, t)

    def to_left(c, d):
        return remote(G[c].at[d], from_right[c].at[d], gS.at[c, d], gR.at[c, d], left, t)

    def grads(c):
        for d in order:
            term = lax.dot_general(
                X[1, :, :, d * deep:(d + 1) * deep].reshape(tokens, deep),
                H[c][1],
                (((0,), (0,)), ((), ())),
                preferred_element_type=F32,
            )
            G[c][d] = term.astype(BF16).reshape(B, Rw, parts[c])
            if d > 0:

                @pl.when(h == 0)
                def _():
                    to_right(c, d).start()

            if d < L - 1:

                @pl.when(far == 0)
                def _():
                    to_left(c, d).start()

    def add_left(c, d):
        remote(from_left[c].at[d], from_left[c].at[d], gS.at[c, d], gL.at[c, d], left, t).wait_recv()
        G[c][d] = (G[c][d].astype(F32) + from_left[c][d].astype(F32)).astype(BF16)

    def add_right(c, d):
        remote(from_right[c].at[d], from_right[c].at[d], gS.at[c, d], gR.at[c, d], right, t).wait_recv()
        G[c][d] = (G[c][d].astype(F32) + from_right[c][d].astype(F32)).astype(BF16)

    def grad_out(c, i, q):
        return remote(
            G[c].at[h, q], gout.at[:, cols(p, c)], hS.at[c, i], hR.at[c, p], dev(q), t
        )

    def sum_step(c, s):
        if s < L - 1:

            @pl.when(jnp.logical_and(has_left, h <= s))
            def _():
                add_left(c, far - s + 2 * h)
                to_right(c, far - s + 2 * h).start()

            @pl.when(jnp.logical_and(has_right, far <= s))
            def _():
                add_right(c, s - far)
                to_left(c, s - far).start()

        else:

            @pl.when(has_left)
            def _():
                add_left(c, h)

            @pl.when(has_right)
            def _():
                add_right(c, h)

            for i, q in enumerate(peers):
                grad_out(c, i, q).start()
            gout[:, cols(p, c)] = G[c][h, p]

    def columns(k):
        return pl.ds(pl.multiple_of(k * deep, deep), deep)

    def tp_out(o, i, m, k):
        return remote(
            O.at[o, :, chunk(m), columns(k)], tp_in.at[o, t, :, :, columns(k)],
            tS.at[o, i, k], tR.at[o, t, k], f, m,
        )

    def tp_got(o, i, m, k):
        there = tp_in.at[o, m, :, :, columns(k)]
        return remote(there, there, tS.at[o, i, k], tR.at[o, m, k], f, m)

    def by_near(o, k):
        return o == 0 or k % 2 == 0

    def first_out(o, k):
        src = S.at[o, :, 1 - b] if by_near(o, k) else S.at[o, 1 - a]
        return remote(
            src.at[:, :, columns(k)], near_in.at[o, :, :, columns(k)],
            nS.at[o, k], nR.at[o, k], dev(near if by_near(o, k) else over), t,
        )

    def second_out(o, k):
        src = S.at[o, 1 - a, b] if by_near(o, k) else S.at[o, a, 1 - b]
        return remote(
            src.at[:, columns(k)], far_in.at[o, :, columns(k)],
            mS.at[o, k], mR.at[o, k], dev(over if by_near(o, k) else near), t,
        )

    def spread(o, pc, k):
        part = 0.0
        for c in range(Q):
            block = W[c][pc, k].reshape(deep, parts[c])
            part += lax.dot_general(
                H[c][o], block, (((1,), (1,)), ((), ())), preferred_element_type=F32
            )
        O[o, :, :, columns(k)] = part.astype(BF16).reshape(B, rows, deep)
        for i, m in enumerate(mates):
            tp_out(o, i, m, k).start()

    def tp_sums(o, k):
        for i, m in enumerate(mates):
            tp_got(o, i, m, k).wait_recv()
        for first in (True, False):
            for other in range(2):
                if by_near(o, k):
                    aa, bb = other, 1 - b if first else b
                else:
                    aa, bb = 1 - a if first else a, other
                total = O[o, 2 * aa + bb, chunk(t), columns(k)].astype(F32)
                for m in mates:
                    total = total + tp_in[o, m, 2 * aa + bb, :, columns(k)].astype(F32)
                S[o, aa, bb, :, columns(k)] = total.astype(BF16)
            if first:
                first_out(o, k).start()

    def near_sums(o, k):
        first_out(o, k).wait_recv()
        for first in (True, False):
            if by_near(o, k):
                aa, bb = 1 - a if first else a, b
                got = aa
            else:
                aa, bb = a, 1 - b if first else b
                got = bb
            total = S[o, aa, bb, :, columns(k)].astype(F32) + near_in[o, got, :, columns(k)].astype(F32)
            S[o, aa, bb, :, columns(k)] = total.astype(BF16)
            if first:
                second_out(o, k).start()

    outs = (out, ing)

    def share(o, i, m):
        there = outs[o].at[chunk(t)]
        return remote(there, there, fS.at[o, i], fR.at[o, t], f, m)

    def shared(o, i, m):
        there = outs[o].at[chunk(m)]
        return remote(there, there, fS.at[o, i], fR.at[o, m], f, m)

    def finish(o):
        for k in range(K):
            second_out(o, k).wait_recv()
            total = S[o, a, b, :, columns(k)].astype(F32) + far_in[o, :, columns(k)].astype(F32)
            outs[o][chunk(t), columns(k)] = total.astype(BF16)
        for i, m in enumerate(mates):
            share(o, i, m).start()

    def slices(c):
        for pc in range(2):
            if (c, pc) == (0, 1) and weights[1] is turned:
                turned[...] = down[...].T
            for i, q in enumerate(peers):
                slice_out(c, pc, i, q).start()

    def pieces(c):
        for pc in range(2):
            push(c, pc, p)

    def keep_own():
        for c, pc in stages:
            own_w(c, pc)
        for j in range(3):
            X[j, p] = acts[j][...]

    def settle(j):
        for i, q in enumerate(peers):
            for o, m in enumerate(mates):
                act_shared(j, i, q, o, m).wait_recv()

    def some(work):
        def run(o, k):
            for part in range(k * K // 4, (k + 1) * K // 4):
                work(o, part)

        return run

    def reach(at, work):
        for s in range((at - 1) * (L - 1) // 3 + 1, at * (L - 1) // 3 + 1) if at else (0,):
            if s == 0:
                work(h)
                continue

            @pl.when(h >= s)
            def _():
                work(h - s)

            @pl.when(far >= s)
            def _():
                work(h + s)

    def steps(work):
        def run(*args):
            at = args[-1]
            for s in range((at - 1) * (L - 1) // 3, at * (L - 1) // 3):
                work(*args[:-1], s + 1)

        return run

    by_part = {
        "slices": slices, "pieces": pieces, "collect": collect, "relay": steps(relay), "sums": steps(sum_step),
        "forward": forward, "backward": backward, "grads": grads,
    }
    others = {
        "over": lambda j: act_out(j, 1, over).start(),
        "near": lambda j: act_out(j, 0, near).start(),
        "take": take, "settle": settle, "keep_own": keep_own, "finish": finish,
        "spread_at": lambda s: reach(s, lambda k: spread(0, 1, k)),
        "tp_at": lambda s: reach(s, lambda k: tp_sums(0, k)),
        "near_at": lambda s: reach(s, lambda k: near_sums(0, k)),
        "spread": some(lambda o, k: spread(o, 1 - o, k)),
        "tp_sums": some(tp_sums), "near_sums": some(near_sums),
    }
    for name, *args in SCHEDULE:
        if name in others:
            others[name](*args)
        elif args[0] < Q:
            by_part[name](*args)

    for i, q in enumerate(peers):
        for c in range(Q):
            there = gout.at[:, cols(q, c)]
            remote(there, there, hS.at[c, i], hR.at[c, q], dev(q), t).wait_recv()
            grad_out(c, i, q).wait_send()
            for pc in range(2):
                slice_out(c, pc, i, q).wait_send()
        for j in range(3):
            for o, m in enumerate(mates):
                act_share(j, i, q, o, m).wait_send()
    for j in range(3):
        act_out(j, 0, near).wait_send()
        act_out(j, 1, over).wait_send()
        act_on(j).wait_send()
    for o in range(2):
        for k in range(K):
            first_out(o, k).wait_send()
            second_out(o, k).wait_send()
        for i, m in enumerate(mates):
            for k in range(K):
                tp_out(o, i, m, k).wait_send()
            share(o, i, m).wait_send()
            shared(o, i, m).wait_recv()
    for c in range(Q):
        for k in range(L):
            @pl.when(h < k)
            def _(c=c, k=k):
                to_right(c, k).wait_send()

            @pl.when(h > k)
            def _(c=c, k=k):
                to_left(c, k).wait_send()

        for pc in range(2):
            for s in range(L):

                @pl.when(jnp.logical_and(has_right, h >= s))
                def _(c=c, pc=pc, s=s):
                    line(c, pc, h - s, 0).wait_send()

                @pl.when(jnp.logical_and(has_left, far >= s))
                def _(c=c, pc=pc, s=s):
                    line(c, pc, h + s, 1).wait_send()


def widths(whole):
    return PARTS if whole == sum(PARTS) else [whole]


def per_device(n, T, fwd_input, saved_input, out_cotangent, up_weight, down_weight, up_grad_sum):
    rows, D = fwd_input.shape
    Rw, F = up_weight.shape
    B = 4
    L, Fs, C = n // B, F // B, rows // T
    parts = widths(Fs)
    Q = len(parts)
    K = D // (B * Rw)
    down = down_weight if Rw % 128 == 0 and down_weight.shape != up_weight.shape else down_weight.T
    dma = pltpu.SemaphoreType.DMA
    mate = max(T - 1, 1)
    flops = 12 * B * rows * Fs * D
    vmem = pl.BlockSpec(memory_space=pltpu.VMEM)
    layer_out, input_grad, grad = pl.pallas_call(
        functools.partial(kernel, n, T, B, parts),
        out_shape=(
            jax.ShapeDtypeStruct((rows, D), BF16),
            jax.ShapeDtypeStruct((rows, D), BF16),
            jax.ShapeDtypeStruct((Rw, F), BF16),
        ),
        in_specs=[vmem] * 5,
        out_specs=(vmem,) * 3,
        scratch_shapes=[
            pltpu.VMEM((3, B, rows, D), BF16),
            pltpu.VMEM((Rw, F), BF16),
            pltpu.VMEM((2, B, rows, D), BF16),
            pltpu.VMEM((2, T, B, C, D), BF16),
            pltpu.VMEM((2, 2, 2, C, D), BF16),
            pltpu.VMEM((2, 2, C, D), BF16),
            pltpu.VMEM((2, C, D), BF16),
            [pltpu.VMEM((2, L, B, Rw, wide), BF16) for wide in parts],
            [pltpu.VMEM((2, B * rows, wide), BF16) for wide in parts],
            [pltpu.VMEM((B * rows, wide), F32) for wide in parts],
            [pltpu.VMEM((L, B, Rw, wide), BF16) for wide in parts],
            [pltpu.VMEM((L, B, Rw, wide), BF16) for wide in parts],
            [pltpu.VMEM((L, B, Rw, wide), BF16) for wide in parts],
            dma((Q, 2, 3)), dma((Q, 2, B)),
            dma((2, Q, 2, L)), dma((Q, 2, L)),
            dma((3, 3)), dma((3, B)),
            dma((3, 3, mate)), dma((3, B, T)),
            dma((2, mate, K)), dma((2, T, K)),
            dma((2, K)), dma((2, K)),
            dma((2, K)), dma((2, K)),
            dma((2, mate)), dma((2, T)),
            dma((Q, L)), dma((Q, L)), dma((Q, L)),
            dma((Q, 3)), dma((Q, B)),
        ],
        compiler_params=pltpu.CompilerParams(
            collective_id=0, has_side_effects=True, vmem_limit_bytes=58 * 2**20
        ),
        cost_estimate=pl.CostEstimate(flops=flops, bytes_accessed=2**25, transcendentals=0),
    )(fwd_input, saved_input, out_cotangent, up_weight, down)
    grad_part = grad.astype(F32)
    grad_scale = float(rows * n) ** (-0.5)
    return (layer_out, input_grad, up_grad_sum + grad_part * grad_scale)


def solution(mesh):
    placed = (
        P("fs", None),
        P("fs", None),
        P("fs", None),
        P("fs", "tp"),
        P("tp", "fs"),
        P("fs", "tp"),
    )
    return jax.shard_map(
        functools.partial(per_device, mesh.shape["fs"], mesh.shape["tp"]),
        mesh=mesh,
        in_specs=placed,
        out_specs=(P("fs", None), P("fs", None), P("fs", "tp")),
        check_vma=False,
    )
```

```python
import functools

import jax
import jax.numpy as jnp
from jax import lax
from jax.experimental import pallas as pl
from jax.experimental.pallas import tpu as pltpu
from jax.sharding import PartitionSpec as P

MESH = pl.DeviceIdType.MESH
F32 = jnp.float32
BF16 = jnp.bfloat16
SPLIT = 2
PARTS = [256, 128, 128]
SCHEDULE = [('slices', 0), ('pieces', 0), ('pieces', 1), ('slices', 1), ('slices', 2), ('collect', 0, 0), ('over', 1), ('collect', 0, 1), ('relay', 0, 0, 1), ('relay', 0, 1, 1), ('near', 1), ('near', 2), ('pieces', 2), ('near', 0), ('over', 2), ('over', 0), ('take', 2, 1), ('collect', 1, 0), ('relay', 0, 0, 2), ('relay', 0, 0, 3), ('take', 1, 0), ('take', 0, 1), ('relay', 0, 1, 2), ('collect', 1, 1), ('keep_own',), ('collect', 2, 0), ('take', 1, 1), ('collect', 2, 1), ('relay', 0, 1, 3), ('relay', 1, 0, 1), ('take', 2, 0), ('take', 1, 2), ('take', 2, 2), ('settle', 1), ('settle', 2), ('take', 0, 0), ('backward', 0), ('grads', 0), ('relay', 1, 0, 2), ('relay', 2, 0, 1), ('relay', 1, 0, 3), ('relay', 1, 1, 1), ('relay', 1, 1, 2), ('take', 0, 2), ('relay', 1, 1, 3), ('settle', 0), ('backward', 1), ('grads', 1), ('forward', 0), ('forward', 1), ('relay', 2, 0, 2), ('relay', 2, 0, 3), ('forward', 2), ('relay', 2, 1, 1), ('spread_at', 0), ('spread_at', 1), ('relay', 2, 1, 2), ('tp_at', 0), ('tp_at', 1), ('spread_at', 2), ('relay', 2, 1, 3), ('backward', 2), ('tp_at', 2), ('sums', 0, 1), ('sums', 0, 2), ('spread', 1, 0), ('spread', 1, 1), ('tp_sums', 1, 0), ('grads', 2), ('spread_at', 3), ('spread', 1, 2), ('tp_at', 3), ('tp_sums', 1, 1), ('near_at', 2), ('near_at', 0), ('sums', 1, 1), ('spread', 1, 3), ('tp_sums', 1, 3), ('near_at', 1), ('tp_sums', 1, 2), ('near_sums', 1, 1), ('sums', 1, 2), ('near_at', 3), ('near_sums', 1, 2), ('near_sums', 1, 0), ('sums', 2, 1), ('sums', 0, 3), ('near_sums', 1, 3), ('sums', 1, 3), ('sums', 2, 2), ('sums', 2, 3), ('finish', 0), ('finish', 1)]


def remote(src, dst, send_sem, recv_sem, fs, tp):
    return pltpu.make_async_remote_copy(
        src_ref=src,
        dst_ref=dst,
        send_sem=send_sem,
        recv_sem=recv_sem,
        device_id=(fs, tp),
        device_id_type=MESH,
    )


def kernel(
    n, T, B, parts, fwd, saved, cot, up, down, out, ing, gout,
    X, turned, O, tp_in, S, near_in, far_in, W, H, pre, G, from_left, from_right,
    wS, wR, zS, zR, aS, aR, bS, bR, tS, tR, nS, nR, mS, mR, fS, fR,
    gS, gL, gR, hS, hR,
):
    L = n // B
    f, t = lax.axis_index("fs"), lax.axis_index("tp")
    h, p = lax.div(f, B), lax.rem(f, B)
    far = L - 1 - h
    rows, D = fwd.shape
    C = rows // T
    Rw, F = up.shape
    Fs = F // B
    Q = len(parts)
    tokens = B * rows
    deep = B * Rw
    K = D // deep
    a, b = lax.div(p, 2), lax.rem(p, 2)
    near, over, cross = 2 * a + 1 - b, 2 * (1 - a) + b, 2 * (1 - a) + 1 - b
    peers = [near, over, cross]
    mates = [lax.rem(t + i, T) for i in range(1, T)]
    has_left, has_right = h > 0, h < L - 1
    stages = [(c, pc) for c in range(Q) for pc in range(2)]

    left, right = f - B, f + B

    def dev(q):
        return h * B + q

    def chunk(index):
        return pl.ds(pl.multiple_of(index * C, C), C)

    def cols(index, c):
        return pl.ds(pl.multiple_of(index * Fs + sum(parts[:c]), 128), parts[c])

    barrier = pltpu.get_barrier_semaphore()
    for q in peers:
        pl.semaphore_signal(barrier, inc=1, device_id=(dev(q), t), device_id_type=MESH)
    for m in mates:
        pl.semaphore_signal(barrier, inc=1, device_id=(f, m), device_id_type=MESH)

    @pl.when(has_left)
    def _():
        pl.semaphore_signal(barrier, inc=1, device_id=(left, t), device_id_type=MESH)

    @pl.when(has_right)
    def _():
        pl.semaphore_signal(barrier, inc=1, device_id=(right, t), device_id_type=MESH)

    ends = lax.div(h + L - 1, L) + lax.div(far + L - 1, L)
    pl.semaphore_wait(barrier, len(peers) + T - 1 + ends)

    weights = (up, down if down.shape == up.shape else turned)

    def slice_out(c, pc, i, q):
        return remote(
            weights[pc].at[:, cols(q, c)], W[c].at[pc, h, p],
            wS.at[c, pc, i], wR.at[c, pc, p], dev(q), t,
        )

    def slice_in(c, pc, q):
        there = W[c].at[pc, h, q]
        return remote(there, there, wS.at[c, pc, 0], wR.at[c, pc, q], dev(q), t)

    def line_piece(c, pc, q, way):
        src = weights[pc].at[:, cols(p, c)] if q is p else W[c].at[pc, h, q]
        return remote(
            src, W[c].at[pc, h, q], zS.at[way, c, pc, h], zR.at[c, pc, h], right if way == 0 else left, t
        )

    def line(c, pc, k, way):
        block = W[c].at[pc, k]
        return remote(
            block, block, zS.at[way, c, pc, k], zR.at[c, pc, k], right if way == 0 else left, t
        )

    def push(c, pc, q):
        @pl.when(has_right)
        def _():
            line_piece(c, pc, q, 0).start()

        @pl.when(has_left)
        def _():
            line_piece(c, pc, q, 1).start()

    def own_w(c, pc):
        W[c][pc, h, p] = weights[pc][:, cols(p, c)]

    def collect(c, pc):
        for q in peers:
            slice_in(c, pc, q).wait_recv()
            push(c, pc, q)

    acts = (fwd, saved, cot)

    def act_out(j, i, q):
        return remote(acts[j].at[chunk(t)], X.at[j, p, chunk(t)], aS.at[j, i], aR.at[j, p], dev(q), t)

    def act_on(j):
        q, to = (over, near) if j == 1 else (near, over)
        there = X.at[j, q, chunk(t)]
        return remote(there, there, aS.at[j, 2], aR.at[j, q], dev(to), t)

    def act_in(j, q):
        there = X.at[j, q, chunk(t)]
        return remote(there, there, aS.at[j, 0], aR.at[j, q], dev(q), t)

    def act_share(j, i, q, o, m):
        there = X.at[j, q, chunk(t)]
        return remote(there, there, bS.at[j, i, o], bR.at[j, q, t], f, m)

    def act_shared(j, i, q, o, m):
        there = X.at[j, q, chunk(m)]
        return remote(there, there, bS.at[j, i, o], bR.at[j, q, m], f, m)

    def take(j, i):
        act_in(j, peers[i]).wait_recv()
        if i == (1 if j == 1 else 0):
            act_on(j).start()
        for o, m in enumerate(mates):
            act_share(j, i, peers[i], o, m).start()

    def relay(c, pc, s):
        @pl.when(h >= s)
        def _():
            line(c, pc, h - s, 0).wait_recv()

            @pl.when(has_right)
            def _():
                line(c, pc, h - s, 0).start()

        @pl.when(far >= s)
        def _():
            line(c, pc, h + s, 1).wait_recv()

            @pl.when(has_left)
            def _():
                line(c, pc, h + s, 1).start()

    def product(c, j, pc):
        return jnp.dot(
            X[j].reshape(tokens, D), W[c][pc].reshape(D, parts[c]), preferred_element_type=F32
        )

    def forward(c):
        positive = jnp.maximum(product(c, 0, 0), 0.0)
        H[c][0] = (positive * positive).astype(BF16)

    def backward(c):
        pre[c][...] = product(c, 1, 0)
        d_hidden = product(c, 2, 1)
        H[c][1] = (d_hidden * 2.0 * jnp.maximum(pre[c][...], 0.0)).astype(BF16)

    order = []
    for i in range((L + 1) // 2):
        order += [L - 1 - i] if L - 1 - i == i else [L - 1 - i, i]

    def to_right(c, d):
        return remote(G[c].at[d], from_left[c].at[d], gS.at[c, d], gL.at[c, d], right, t)

    def to_left(c, d):
        return remote(G[c].at[d], from_right[c].at[d], gS.at[c, d], gR.at[c, d], left, t)

    def grads(c):
        for d in order:
            term = lax.dot_general(
                X[1, :, :, d * deep:(d + 1) * deep].reshape(tokens, deep),
                H[c][1],
                (((0,), (0,)), ((), ())),
                preferred_element_type=F32,
            )
            G[c][d] = term.astype(BF16).reshape(B, Rw, parts[c])
            if d > 0:

                @pl.when(h == 0)
                def _():
                    to_right(c, d).start()

            if d < L - 1:

                @pl.when(far == 0)
                def _():
                    to_left(c, d).start()

    def add_left(c, d):
        remote(from_left[c].at[d], from_left[c].at[d], gS.at[c, d], gL.at[c, d], left, t).wait_recv()
        G[c][d] = (G[c][d].astype(F32) + from_left[c][d].astype(F32)).astype(BF16)

    def add_right(c, d):
        remote(from_right[c].at[d], from_right[c].at[d], gS.at[c, d], gR.at[c, d], right, t).wait_recv()
        G[c][d] = (G[c][d].astype(F32) + from_right[c][d].astype(F32)).astype(BF16)

    def grad_out(c, i, q):
        return remote(
            G[c].at[h, q], gout.at[:, cols(p, c)], hS.at[c, i], hR.at[c, p], dev(q), t
        )

    def sum_step(c, s):
        if s < L - 1:

            @pl.when(jnp.logical_and(has_left, h <= s))
            def _():
                add_left(c, far - s + 2 * h)
                to_right(c, far - s + 2 * h).start()

            @pl.when(jnp.logical_and(has_right, far <= s))
            def _():
                add_right(c, s - far)
                to_left(c, s - far).start()

        else:

            @pl.when(has_left)
            def _():
                add_left(c, h)

            @pl.when(has_right)
            def _():
                add_right(c, h)

            for i, q in enumerate(peers):
                grad_out(c, i, q).start()
            gout[:, cols(p, c)] = G[c][h, p]

    def columns(k):
        return pl.ds(pl.multiple_of(k * deep, deep), deep)

    def tp_out(o, i, m, k):
        return remote(
            O.at[o, :, chunk(m), columns(k)], tp_in.at[o, t, :, :, columns(k)],
            tS.at[o, i, k], tR.at[o, t, k], f, m,
        )

    def tp_got(o, i, m, k):
        there = tp_in.at[o, m, :, :, columns(k)]
        return remote(there, there, tS.at[o, i, k], tR.at[o, m, k], f, m)

    def by_near(o, k):
        return o == 0 or k % 2 == 0

    def first_out(o, k):
        src = S.at[o, :, 1 - b] if by_near(o, k) else S.at[o, 1 - a]
        return remote(
            src.at[:, :, columns(k)], near_in.at[o, :, :, columns(k)],
            nS.at[o, k], nR.at[o, k], dev(near if by_near(o, k) else over), t,
        )

    def second_out(o, k):
        src = S.at[o, 1 - a, b] if by_near(o, k) else S.at[o, a, 1 - b]
        return remote(
            src.at[:, columns(k)], far_in.at[o, :, columns(k)],
            mS.at[o, k], mR.at[o, k], dev(over if by_near(o, k) else near), t,
        )

    def spread(o, pc, k):
        units = jnp.concatenate([H[c][o] for c in range(Q)], axis=1)
        block = jnp.concatenate([W[c][pc, k].reshape(deep, parts[c]) for c in range(Q)], axis=1)
        part = lax.dot_general(units, block, (((1,), (1,)), ((), ())), preferred_element_type=F32)
        O[o, :, :, columns(k)] = part.astype(BF16).reshape(B, rows, deep)
        for i, m in enumerate(mates):
            tp_out(o, i, m, k).start()

    def tp_sums(o, k):
        for i, m in enumerate(mates):
            tp_got(o, i, m, k).wait_recv()
        for first in (True, False):
            for other in range(2):
                if by_near(o, k):
                    aa, bb = other, 1 - b if first else b
                else:
                    aa, bb = 1 - a if first else a, other
                total = O[o, 2 * aa + bb, chunk(t), columns(k)].astype(F32)
                for m in mates:
                    total = total + tp_in[o, m, 2 * aa + bb, :, columns(k)].astype(F32)
                S[o, aa, bb, :, columns(k)] = total.astype(BF16)
            if first:
                first_out(o, k).start()

    def near_sums(o, k):
        first_out(o, k).wait_recv()
        for first in (True, False):
            if by_near(o, k):
                aa, bb = 1 - a if first else a, b
                got = aa
            else:
                aa, bb = a, 1 - b if first else b
                got = bb
            total = S[o, aa, bb, :, columns(k)].astype(F32) + near_in[o, got, :, columns(k)].astype(F32)
            S[o, aa, bb, :, columns(k)] = total.astype(BF16)
            if first:
                second_out(o, k).start()

    outs = (out, ing)

    def share(o, i, m):
        there = outs[o].at[chunk(t)]
        return remote(there, there, fS.at[o, i], fR.at[o, t], f, m)

    def shared(o, i, m):
        there = outs[o].at[chunk(m)]
        return remote(there, there, fS.at[o, i], fR.at[o, m], f, m)

    def finish(o):
        for k in range(K):
            second_out(o, k).wait_recv()
            total = S[o, a, b, :, columns(k)].astype(F32) + far_in[o, :, columns(k)].astype(F32)
            outs[o][chunk(t), columns(k)] = total.astype(BF16)
        for i, m in enumerate(mates):
            share(o, i, m).start()

    def slices(c):
        for pc in range(2):
            if (c, pc) == (0, 1) and weights[1] is turned:
                turned[...] = down[...].T
            for i, q in enumerate(peers):
                slice_out(c, pc, i, q).start()

    def pieces(c):
        for pc in range(2):
            push(c, pc, p)

    def keep_own():
        for c, pc in stages:
            own_w(c, pc)
        for j in range(3):
            X[j, p] = acts[j][...]

    def settle(j):
        for i, q in enumerate(peers):
            for o, m in enumerate(mates):
                act_shared(j, i, q, o, m).wait_recv()

    def some(work):
        def run(o, k):
            for part in range(k * K // 4, (k + 1) * K // 4):
                work(o, part)

        return run

    def reach(at, work):
        for s in range((at - 1) * (L - 1) // 3 + 1, at * (L - 1) // 3 + 1) if at else (0,):
            if s == 0:
                work(h)
                continue

            @pl.when(h >= s)
            def _():
                work(h - s)

            @pl.when(far >= s)
            def _():
                work(h + s)

    def steps(work):
        def run(*args):
            at = args[-1]
            for s in range((at - 1) * (L - 1) // 3, at * (L - 1) // 3):
                work(*args[:-1], s + 1)

        return run

    by_part = {
        "slices": slices, "pieces": pieces, "collect": collect, "relay": steps(relay), "sums": steps(sum_step),
        "forward": forward, "backward": backward, "grads": grads,
    }
    others = {
        "over": lambda j: act_out(j, 1, over).start(),
        "near": lambda j: act_out(j, 0, near).start(),
        "take": take, "settle": settle, "keep_own": keep_own, "finish": finish,
        "spread_at": lambda s: reach(s, lambda k: spread(0, 1, k)),
        "tp_at": lambda s: reach(s, lambda k: tp_sums(0, k)),
        "near_at": lambda s: reach(s, lambda k: near_sums(0, k)),
        "spread": some(lambda o, k: spread(o, 1 - o, k)),
        "tp_sums": some(tp_sums), "near_sums": some(near_sums),
    }
    for name, *args in SCHEDULE:
        if name in others:
            others[name](*args)
        elif args[0] < Q:
            by_part[name](*args)

    for i, q in enumerate(peers):
        for c in range(Q):
            there = gout.at[:, cols(q, c)]
            remote(there, there, hS.at[c, i], hR.at[c, q], dev(q), t).wait_recv()
            grad_out(c, i, q).wait_send()
            for pc in range(2):
                slice_out(c, pc, i, q).wait_send()
        for j in range(3):
            for o, m in enumerate(mates):
                act_share(j, i, q, o, m).wait_send()
    for j in range(3):
        act_out(j, 0, near).wait_send()
        act_out(j, 1, over).wait_send()
        act_on(j).wait_send()
    for o in range(2):
        for k in range(K):
            first_out(o, k).wait_send()
            second_out(o, k).wait_send()
        for i, m in enumerate(mates):
            for k in range(K):
                tp_out(o, i, m, k).wait_send()
            share(o, i, m).wait_send()
            shared(o, i, m).wait_recv()
    for c in range(Q):
        for k in range(L):
            @pl.when(h < k)
            def _(c=c, k=k):
                to_right(c, k).wait_send()

            @pl.when(h > k)
            def _(c=c, k=k):
                to_left(c, k).wait_send()

        for pc in range(2):
            for s in range(L):

                @pl.when(jnp.logical_and(has_right, h >= s))
                def _(c=c, pc=pc, s=s):
                    line(c, pc, h - s, 0).wait_send()

                @pl.when(jnp.logical_and(has_left, far >= s))
                def _(c=c, pc=pc, s=s):
                    line(c, pc, h + s, 1).wait_send()


def hand_over(scale, out, ing, grad, running, out_to, ing_to, grad_to, o, i, g, r, total, came, went):
    def pieces(src, dst, sem):
        size = src.shape[0] // SPLIT
        return [
            pltpu.make_async_copy(src.at[pl.ds(at * size, size)], dst.at[pl.ds(at * size, size)], sem.at[at])
            for at in range(SPLIT)
        ]

    ins = [
        pieces(src, dst, came.at[at])
        for at, (src, dst) in enumerate(((running, r), (grad, g), (out, o), (ing, i)))
    ]
    outs = [
        pieces(src, dst, went.at[at])
        for at, (src, dst) in enumerate(((total, grad_to), (o, out_to), (i, ing_to)))
    ]
    for at in range(SPLIT):
        for copies in ins:
            copies[at].start()
    size = total.shape[0] // SPLIT
    for at in range(SPLIT):
        part = pl.ds(at * size, size)
        ins[0][at].wait()
        ins[1][at].wait()
        total[part] = r[part] + g[part].astype(F32) * scale
        outs[0][at].start()
        for copies in (1, 2):
            ins[copies + 1][at].wait()
            outs[copies][at].start()
    for copies in outs:
        for copy in copies:
            copy.wait()


def widths(whole):
    return PARTS if whole == sum(PARTS) else [whole]


def per_device(n, T, fwd_input, saved_input, out_cotangent, up_weight, down_weight, up_grad_sum):
    rows, D = fwd_input.shape
    Rw, F = up_weight.shape
    B = 4
    L, Fs, C = n // B, F // B, rows // T
    parts = widths(Fs)
    Q = len(parts)
    K = D // (B * Rw)
    down = down_weight if Rw % 128 == 0 and down_weight.shape != up_weight.shape else down_weight.T
    dma = pltpu.SemaphoreType.DMA
    mate = max(T - 1, 1)
    flops = 12 * B * rows * Fs * D
    vmem = pl.BlockSpec(memory_space=pltpu.VMEM)
    layer_out, input_grad, grad = pl.pallas_call(
        functools.partial(kernel, n, T, B, parts),
        out_shape=(
            jax.ShapeDtypeStruct((rows, D), BF16),
            jax.ShapeDtypeStruct((rows, D), BF16),
            jax.ShapeDtypeStruct((Rw, F), BF16),
        ),
        in_specs=[vmem] * 5,
        out_specs=(vmem,) * 3,
        scratch_shapes=[
            pltpu.VMEM((3, B, rows, D), BF16),
            pltpu.VMEM((Rw, F), BF16),
            pltpu.VMEM((2, B, rows, D), BF16),
            pltpu.VMEM((2, T, B, C, D), BF16),
            pltpu.VMEM((2, 2, 2, C, D), BF16),
            pltpu.VMEM((2, 2, C, D), BF16),
            pltpu.VMEM((2, C, D), BF16),
            [pltpu.VMEM((2, L, B, Rw, wide), BF16) for wide in parts],
            [pltpu.VMEM((2, B * rows, wide), BF16) for wide in parts],
            [pltpu.VMEM((B * rows, wide), F32) for wide in parts],
            [pltpu.VMEM((L, B, Rw, wide), BF16) for wide in parts],
            [pltpu.VMEM((L, B, Rw, wide), BF16) for wide in parts],
            [pltpu.VMEM((L, B, Rw, wide), BF16) for wide in parts],
            dma((Q, 2, 3)), dma((Q, 2, B)),
            dma((2, Q, 2, L)), dma((Q, 2, L)),
            dma((3, 3)), dma((3, B)),
            dma((3, 3, mate)), dma((3, B, T)),
            dma((2, mate, K)), dma((2, T, K)),
            dma((2, K)), dma((2, K)),
            dma((2, K)), dma((2, K)),
            dma((2, mate)), dma((2, T)),
            dma((Q, L)), dma((Q, L)), dma((Q, L)),
            dma((Q, 3)), dma((Q, B)),
        ],
        compiler_params=pltpu.CompilerParams(
            collective_id=0, has_side_effects=True, vmem_limit_bytes=58 * 2**20
        ),
        cost_estimate=pl.CostEstimate(flops=flops, bytes_accessed=2**25, transcendentals=0),
    )(fwd_input, saved_input, out_cotangent, up_weight, down)
    grad_scale = float(rows * n) ** (-0.5)
    anywhere = pl.BlockSpec(memory_space=pl.ANY)
    return pl.pallas_call(
        functools.partial(hand_over, grad_scale),
        out_shape=(
            jax.ShapeDtypeStruct((rows, D), BF16),
            jax.ShapeDtypeStruct((rows, D), BF16),
            jax.ShapeDtypeStruct((Rw, F), F32),
        ),
        in_specs=[anywhere] * 4,
        out_specs=(anywhere,) * 3,
        scratch_shapes=[
            pltpu.VMEM((rows, D), BF16),
            pltpu.VMEM((rows, D), BF16),
            pltpu.VMEM((Rw, F), BF16),
            pltpu.VMEM((Rw, F), F32),
            pltpu.VMEM((Rw, F), F32),
            dma((4, SPLIT)), dma((3, SPLIT)),
        ],
        cost_estimate=pl.CostEstimate(flops=2 * Rw * F, bytes_accessed=14 * Rw * F, transcendentals=0),
    )(layer_out, input_grad, grad, up_grad_sum)


def solution(mesh):
    placed = (
        P("fs", None),
        P("fs", None),
        P("fs", None),
        P("fs", "tp"),
        P("tp", "fs"),
        P("fs", "tp"),
    )
    return jax.shard_map(
        functools.partial(per_device, mesh.shape["fs"], mesh.shape["tp"]),
        mesh=mesh,
        in_specs=placed,
        out_specs=(P("fs", None), P("fs", None), P("fs", "tp")),
        check_vma=False,
    )
```

```python
import functools

import jax
import jax.numpy as jnp
from jax import lax
from jax.experimental import pallas as pl
from jax.experimental.pallas import tpu as pltpu
from jax.sharding import PartitionSpec as P

MESH = pl.DeviceIdType.MESH
F32 = jnp.float32
BF16 = jnp.bfloat16
SPLIT = 2
PARTS = [256, 128, 128]
SCHEDULE = [('slices', 0), ('keep_own',), ('pieces', 0), ('near', 2), ('slices', 1), ('pieces', 1), ('collect', 0, 0), ('over', 1), ('collect', 0, 1), ('relay', 0, 0, 1), ('relay', 0, 1, 1), ('over', 0), ('near', 1), ('relay', 0, 0, 2), ('collect', 1, 0), ('slices', 2), ('relay', 0, 1, 2), ('over', 2), ('collect', 1, 1), ('take', 1, 1), ('relay', 0, 0, 3), ('pieces', 2), ('near', 0), ('collect', 2, 1), ('take', 1, 0), ('take', 2, 1), ('take', 2, 0), ('relay', 1, 0, 1), ('relay', 0, 1, 3), ('take', 2, 2), ('take', 1, 2), ('take', 0, 0), ('settle', 1), ('settle', 2), ('collect', 2, 0), ('relay', 1, 0, 2), ('relay', 1, 1, 1), ('take', 0, 1), ('backward', 0), ('grads', 0), ('take', 0, 2), ('relay', 1, 1, 2), ('relay', 1, 0, 3), ('settle', 0), ('relay', 2, 0, 1), ('forward', 0), ('relay', 1, 1, 3), ('backward', 1), ('grads', 1), ('relay', 2, 0, 2), ('forward', 1), ('relay', 2, 0, 3), ('forward', 2), ('relay', 2, 1, 1), ('spread_at', 0), ('spread_at', 1), ('tp_at', 0), ('tp_at', 1), ('relay', 2, 1, 2), ('spread_at', 2), ('tp_at', 2), ('relay', 2, 1, 3), ('spread_at', 3), ('sums', 0, 1), ('backward', 2), ('spread', 1, 0), ('spread', 1, 3), ('spread', 1, 1), ('tp_sums', 1, 0), ('near_at', 0), ('sums', 1, 1), ('tp_sums', 1, 1), ('tp_at', 3), ('grads', 2), ('spread', 1, 2), ('near_at', 2), ('tp_sums', 1, 3), ('sums', 0, 2), ('sums', 2, 1), ('sums', 1, 2), ('near_sums', 1, 0), ('tp_sums', 1, 2), ('sums', 0, 3), ('near_at', 3), ('near_sums', 1, 1), ('near_sums', 1, 2), ('near_at', 1), ('sums', 2, 2), ('near_sums', 1, 3), ('sums', 1, 3), ('finish', 0), ('sums', 2, 3), ('finish', 1)]


def remote(src, dst, send_sem, recv_sem, fs, tp):
    return pltpu.make_async_remote_copy(
        src_ref=src,
        dst_ref=dst,
        send_sem=send_sem,
        recv_sem=recv_sem,
        device_id=(fs, tp),
        device_id_type=MESH,
    )


def kernel(
    n, T, B, parts, fwd, saved, cot, up, down, out, ing, gout,
    X, turned, O, tp_in, S, near_in, far_in, W, H, pre, G, from_left, from_right,
    wS, wR, zS, zR, aS, aR, bS, bR, tS, tR, nS, nR, mS, mR, fS, fR,
    gS, gL, gR, hS, hR,
):
    L = n // B
    f, t = lax.axis_index("fs"), lax.axis_index("tp")
    h, p = lax.div(f, B), lax.rem(f, B)
    far = L - 1 - h
    rows, D = fwd.shape
    C = rows // T
    Rw, F = up.shape
    Fs = F // B
    Q = len(parts)
    tokens = B * rows
    deep = B * Rw
    K = D // deep
    a, b = lax.div(p, 2), lax.rem(p, 2)
    near, over, cross = 2 * a + 1 - b, 2 * (1 - a) + b, 2 * (1 - a) + 1 - b
    peers = [near, over, cross]
    mates = [lax.rem(t + i, T) for i in range(1, T)]
    has_left, has_right = h > 0, h < L - 1
    stages = [(c, pc) for c in range(Q) for pc in range(2)]

    left, right = f - B, f + B

    def dev(q):
        return h * B + q

    def chunk(index):
        return pl.ds(pl.multiple_of(index * C, C), C)

    def cols(index, c):
        return pl.ds(pl.multiple_of(index * Fs + sum(parts[:c]), 128), parts[c])

    barrier = pltpu.get_barrier_semaphore()
    for q in peers:
        pl.semaphore_signal(barrier, inc=1, device_id=(dev(q), t), device_id_type=MESH)
    for m in mates:
        pl.semaphore_signal(barrier, inc=1, device_id=(f, m), device_id_type=MESH)

    @pl.when(has_left)
    def _():
        pl.semaphore_signal(barrier, inc=1, device_id=(left, t), device_id_type=MESH)

    @pl.when(has_right)
    def _():
        pl.semaphore_signal(barrier, inc=1, device_id=(right, t), device_id_type=MESH)

    ends = lax.div(h + L - 1, L) + lax.div(far + L - 1, L)
    pl.semaphore_wait(barrier, len(peers) + T - 1 + ends)

    weights = (up, down if down.shape == up.shape else turned)

    def slice_out(c, pc, i, q):
        return remote(
            weights[pc].at[:, cols(q, c)], W[c].at[pc, h, p],
            wS.at[c, pc, i], wR.at[c, pc, p], dev(q), t,
        )

    def slice_in(c, pc, q):
        there = W[c].at[pc, h, q]
        return remote(there, there, wS.at[c, pc, 0], wR.at[c, pc, q], dev(q), t)

    def line_piece(c, pc, q, way):
        src = weights[pc].at[:, cols(p, c)] if q is p else W[c].at[pc, h, q]
        return remote(
            src, W[c].at[pc, h, q], zS.at[way, c, pc, h], zR.at[c, pc, h], right if way == 0 else left, t
        )

    def line(c, pc, k, way):
        block = W[c].at[pc, k]
        return remote(
            block, block, zS.at[way, c, pc, k], zR.at[c, pc, k], right if way == 0 else left, t
        )

    def push(c, pc, q):
        @pl.when(has_right)
        def _():
            line_piece(c, pc, q, 0).start()

        @pl.when(has_left)
        def _():
            line_piece(c, pc, q, 1).start()

    def own_w(c, pc):
        W[c][pc, h, p] = weights[pc][:, cols(p, c)]

    def collect(c, pc):
        for q in peers:
            slice_in(c, pc, q).wait_recv()
            push(c, pc, q)

    acts = (fwd, saved, cot)

    def act_out(j, i, q):
        return remote(acts[j].at[chunk(t)], X.at[j, p, chunk(t)], aS.at[j, i], aR.at[j, p], dev(q), t)

    def act_on(j):
        q, to = (over, near) if j == 1 else (near, over)
        there = X.at[j, q, chunk(t)]
        return remote(there, there, aS.at[j, 2], aR.at[j, q], dev(to), t)

    def act_in(j, q):
        there = X.at[j, q, chunk(t)]
        return remote(there, there, aS.at[j, 0], aR.at[j, q], dev(q), t)

    def act_share(j, i, q, o, m):
        there = X.at[j, q, chunk(t)]
        return remote(there, there, bS.at[j, i, o], bR.at[j, q, t], f, m)

    def act_shared(j, i, q, o, m):
        there = X.at[j, q, chunk(m)]
        return remote(there, there, bS.at[j, i, o], bR.at[j, q, m], f, m)

    def take(j, i):
        act_in(j, peers[i]).wait_recv()
        if i == (1 if j == 1 else 0):
            act_on(j).start()
        for o, m in enumerate(mates):
            act_share(j, i, peers[i], o, m).start()

    def relay(c, pc, s):
        @pl.when(h >= s)
        def _():
            line(c, pc, h - s, 0).wait_recv()

            @pl.when(has_right)
            def _():
                line(c, pc, h - s, 0).start()

        @pl.when(far >= s)
        def _():
            line(c, pc, h + s, 1).wait_recv()

            @pl.when(has_left)
            def _():
                line(c, pc, h + s, 1).start()

    def product(c, j, pc):
        return jnp.dot(
            X[j].reshape(tokens, D), W[c][pc].reshape(D, parts[c]), preferred_element_type=F32
        )

    def forward(c):
        positive = jnp.maximum(product(c, 0, 0), 0.0)
        H[c][0] = (positive * positive).astype(BF16)

    def backward(c):
        pre[c][...] = product(c, 1, 0)
        d_hidden = product(c, 2, 1)
        H[c][1] = (d_hidden * 2.0 * jnp.maximum(pre[c][...], 0.0)).astype(BF16)

    order = []
    for i in range((L + 1) // 2):
        order += [L - 1 - i] if L - 1 - i == i else [L - 1 - i, i]

    def to_right(c, d):
        return remote(G[c].at[d], from_left[c].at[d], gS.at[c, d], gL.at[c, d], right, t)

    def to_left(c, d):
        return remote(G[c].at[d], from_right[c].at[d], gS.at[c, d], gR.at[c, d], left, t)

    def grads(c):
        for d in order:
            term = lax.dot_general(
                X[1, :, :, d * deep:(d + 1) * deep].reshape(tokens, deep),
                H[c][1],
                (((0,), (0,)), ((), ())),
                preferred_element_type=F32,
            )
            G[c][d] = term.astype(BF16).reshape(B, Rw, parts[c])
            if d > 0:

                @pl.when(h == 0)
                def _():
                    to_right(c, d).start()

            if d < L - 1:

                @pl.when(far == 0)
                def _():
                    to_left(c, d).start()

    def add_left(c, d):
        remote(from_left[c].at[d], from_left[c].at[d], gS.at[c, d], gL.at[c, d], left, t).wait_recv()
        G[c][d] = (G[c][d].astype(F32) + from_left[c][d].astype(F32)).astype(BF16)

    def add_right(c, d):
        remote(from_right[c].at[d], from_right[c].at[d], gS.at[c, d], gR.at[c, d], right, t).wait_recv()
        G[c][d] = (G[c][d].astype(F32) + from_right[c][d].astype(F32)).astype(BF16)

    def grad_out(c, i, q):
        return remote(
            G[c].at[h, q], gout.at[:, cols(p, c)], hS.at[c, i], hR.at[c, p], dev(q), t
        )

    def sum_step(c, s):
        if s < L - 1:

            @pl.when(jnp.logical_and(has_left, h <= s))
            def _():
                add_left(c, far - s + 2 * h)
                to_right(c, far - s + 2 * h).start()

            @pl.when(jnp.logical_and(has_right, far <= s))
            def _():
                add_right(c, s - far)
                to_left(c, s - far).start()

        else:

            @pl.when(has_left)
            def _():
                add_left(c, h)

            @pl.when(has_right)
            def _():
                add_right(c, h)

            for i, q in enumerate(peers):
                grad_out(c, i, q).start()
            gout[:, cols(p, c)] = G[c][h, p]

    def columns(k):
        return pl.ds(pl.multiple_of(k * deep, deep), deep)

    def tp_out(o, i, m, k):
        return remote(
            O.at[o, :, chunk(m), columns(k)], tp_in.at[o, t, :, :, columns(k)],
            tS.at[o, i, k], tR.at[o, t, k], f, m,
        )

    def tp_got(o, i, m, k):
        there = tp_in.at[o, m, :, :, columns(k)]
        return remote(there, there, tS.at[o, i, k], tR.at[o, m, k], f, m)

    def by_near(o, k):
        return o == 0 or k % 2 == 0

    def first_out(o, k):
        src = S.at[o, :, 1 - b] if by_near(o, k) else S.at[o, 1 - a]
        return remote(
            src.at[:, :, columns(k)], near_in.at[o, :, :, columns(k)],
            nS.at[o, k], nR.at[o, k], dev(near if by_near(o, k) else over), t,
        )

    def second_out(o, k):
        src = S.at[o, 1 - a, b] if by_near(o, k) else S.at[o, a, 1 - b]
        return remote(
            src.at[:, columns(k)], far_in.at[o, :, columns(k)],
            mS.at[o, k], mR.at[o, k], dev(over if by_near(o, k) else near), t,
        )

    def spread(o, pc, k):
        units = jnp.concatenate([H[c][o] for c in range(Q)], axis=1)
        block = jnp.concatenate([W[c][pc, k].reshape(deep, parts[c]) for c in range(Q)], axis=1)
        part = lax.dot_general(units, block, (((1,), (1,)), ((), ())), preferred_element_type=F32)
        O[o, :, :, columns(k)] = part.astype(BF16).reshape(B, rows, deep)
        for i, m in enumerate(mates):
            tp_out(o, i, m, k).start()

    def tp_sums(o, k):
        for i, m in enumerate(mates):
            tp_got(o, i, m, k).wait_recv()
        for first in (True, False):
            for other in range(2):
                if by_near(o, k):
                    aa, bb = other, 1 - b if first else b
                else:
                    aa, bb = 1 - a if first else a, other
                total = O[o, 2 * aa + bb, chunk(t), columns(k)].astype(F32)
                for m in mates:
                    total = total + tp_in[o, m, 2 * aa + bb, :, columns(k)].astype(F32)
                S[o, aa, bb, :, columns(k)] = total.astype(BF16)
            if first:
                first_out(o, k).start()

    def near_sums(o, k):
        first_out(o, k).wait_recv()
        for first in (True, False):
            if by_near(o, k):
                aa, bb = 1 - a if first else a, b
                got = aa
            else:
                aa, bb = a, 1 - b if first else b
                got = bb
            total = S[o, aa, bb, :, columns(k)].astype(F32) + near_in[o, got, :, columns(k)].astype(F32)
            S[o, aa, bb, :, columns(k)] = total.astype(BF16)
            if first:
                second_out(o, k).start()

    outs = (out, ing)

    def share(o, i, m):
        there = outs[o].at[chunk(t)]
        return remote(there, there, fS.at[o, i], fR.at[o, t], f, m)

    def shared(o, i, m):
        there = outs[o].at[chunk(m)]
        return remote(there, there, fS.at[o, i], fR.at[o, m], f, m)

    def finish(o):
        for k in range(K):
            second_out(o, k).wait_recv()
            total = S[o, a, b, :, columns(k)].astype(F32) + far_in[o, :, columns(k)].astype(F32)
            outs[o][chunk(t), columns(k)] = total.astype(BF16)
        for i, m in enumerate(mates):
            share(o, i, m).start()

    def slices(c):
        for pc in range(2):
            if (c, pc) == (0, 1) and weights[1] is turned:
                turned[...] = down[...].T
            for i, q in enumerate(peers):
                slice_out(c, pc, i, q).start()

    def pieces(c):
        for pc in range(2):
            push(c, pc, p)

    def keep_own():
        for c, pc in stages:
            own_w(c, pc)
        for j in range(3):
            X[j, p] = acts[j][...]

    def settle(j):
        for i, q in enumerate(peers):
            for o, m in enumerate(mates):
                act_shared(j, i, q, o, m).wait_recv()

    def some(work):
        def run(o, k):
            for part in range(k * K // 4, (k + 1) * K // 4):
                work(o, part)

        return run

    def reach(at, work):
        for s in range((at - 1) * (L - 1) // 3 + 1, at * (L - 1) // 3 + 1) if at else (0,):
            if s == 0:
                work(h)
                continue

            @pl.when(h >= s)
            def _():
                work(h - s)

            @pl.when(far >= s)
            def _():
                work(h + s)

    def steps(work):
        def run(*args):
            at = args[-1]
            for s in range((at - 1) * (L - 1) // 3, at * (L - 1) // 3):
                work(*args[:-1], s + 1)

        return run

    by_part = {
        "slices": slices, "pieces": pieces, "collect": collect, "relay": steps(relay), "sums": steps(sum_step),
        "forward": forward, "backward": backward, "grads": grads,
    }
    others = {
        "over": lambda j: act_out(j, 1, over).start(),
        "near": lambda j: act_out(j, 0, near).start(),
        "take": take, "settle": settle, "keep_own": keep_own, "finish": finish,
        "spread_at": lambda s: reach(s, lambda k: spread(0, 1, k)),
        "tp_at": lambda s: reach(s, lambda k: tp_sums(0, k)),
        "near_at": lambda s: reach(s, lambda k: near_sums(0, k)),
        "spread": some(lambda o, k: spread(o, 1 - o, k)),
        "tp_sums": some(tp_sums), "near_sums": some(near_sums),
    }
    for name, *args in SCHEDULE:
        if name in others:
            others[name](*args)
        elif args[0] < Q:
            by_part[name](*args)

    for i, q in enumerate(peers):
        for c in range(Q):
            there = gout.at[:, cols(q, c)]
            remote(there, there, hS.at[c, i], hR.at[c, q], dev(q), t).wait_recv()
            grad_out(c, i, q).wait_send()
            for pc in range(2):
                slice_out(c, pc, i, q).wait_send()
        for j in range(3):
            for o, m in enumerate(mates):
                act_share(j, i, q, o, m).wait_send()
    for j in range(3):
        act_out(j, 0, near).wait_send()
        act_out(j, 1, over).wait_send()
        act_on(j).wait_send()
    for o in range(2):
        for k in range(K):
            first_out(o, k).wait_send()
            second_out(o, k).wait_send()
        for i, m in enumerate(mates):
            for k in range(K):
                tp_out(o, i, m, k).wait_send()
            share(o, i, m).wait_send()
            shared(o, i, m).wait_recv()
    for c in range(Q):
        for k in range(L):
            @pl.when(h < k)
            def _(c=c, k=k):
                to_right(c, k).wait_send()

            @pl.when(h > k)
            def _(c=c, k=k):
                to_left(c, k).wait_send()

        for pc in range(2):
            for s in range(L):

                @pl.when(jnp.logical_and(has_right, h >= s))
                def _(c=c, pc=pc, s=s):
                    line(c, pc, h - s, 0).wait_send()

                @pl.when(jnp.logical_and(has_left, far >= s))
                def _(c=c, pc=pc, s=s):
                    line(c, pc, h + s, 1).wait_send()


def hand_over(scale, out, ing, grad, running, out_to, ing_to, grad_to, o, i, g, r, total, came, went):
    def pieces(src, dst, sem):
        size = src.shape[0] // SPLIT
        return [
            pltpu.make_async_copy(src.at[pl.ds(at * size, size)], dst.at[pl.ds(at * size, size)], sem.at[at])
            for at in range(SPLIT)
        ]

    ins = [
        pieces(src, dst, came.at[at])
        for at, (src, dst) in enumerate(((running, r), (grad, g), (out, o), (ing, i)))
    ]
    outs = [
        pieces(src, dst, went.at[at])
        for at, (src, dst) in enumerate(((total, grad_to), (o, out_to), (i, ing_to)))
    ]
    for at in range(SPLIT):
        for copies in ins:
            copies[at].start()
    size = total.shape[0] // SPLIT
    for at in range(SPLIT):
        part = pl.ds(at * size, size)
        ins[0][at].wait()
        ins[1][at].wait()
        total[part] = r[part] + g[part].astype(F32) * scale
        outs[0][at].start()
        for copies in (1, 2):
            ins[copies + 1][at].wait()
            outs[copies][at].start()
    for copies in outs:
        for copy in copies:
            copy.wait()


def widths(whole):
    return PARTS if whole == sum(PARTS) else [whole]


def per_device(n, T, fwd_input, saved_input, out_cotangent, up_weight, down_weight, up_grad_sum):
    rows, D = fwd_input.shape
    Rw, F = up_weight.shape
    B = 4
    L, Fs, C = n // B, F // B, rows // T
    parts = widths(Fs)
    Q = len(parts)
    K = D // (B * Rw)
    down = down_weight if Rw % 128 == 0 and down_weight.shape != up_weight.shape else down_weight.T
    dma = pltpu.SemaphoreType.DMA
    mate = max(T - 1, 1)
    flops = 12 * B * rows * Fs * D
    vmem = pl.BlockSpec(memory_space=pltpu.VMEM)
    layer_out, input_grad, grad = pl.pallas_call(
        functools.partial(kernel, n, T, B, parts),
        out_shape=(
            jax.ShapeDtypeStruct((rows, D), BF16),
            jax.ShapeDtypeStruct((rows, D), BF16),
            jax.ShapeDtypeStruct((Rw, F), BF16),
        ),
        in_specs=[vmem] * 5,
        out_specs=(vmem,) * 3,
        scratch_shapes=[
            pltpu.VMEM((3, B, rows, D), BF16),
            pltpu.VMEM((Rw, F), BF16),
            pltpu.VMEM((2, B, rows, D), BF16),
            pltpu.VMEM((2, T, B, C, D), BF16),
            pltpu.VMEM((2, 2, 2, C, D), BF16),
            pltpu.VMEM((2, 2, C, D), BF16),
            pltpu.VMEM((2, C, D), BF16),
            [pltpu.VMEM((2, L, B, Rw, wide), BF16) for wide in parts],
            [pltpu.VMEM((2, B * rows, wide), BF16) for wide in parts],
            [pltpu.VMEM((B * rows, wide), F32) for wide in parts],
            [pltpu.VMEM((L, B, Rw, wide), BF16) for wide in parts],
            [pltpu.VMEM((L, B, Rw, wide), BF16) for wide in parts],
            [pltpu.VMEM((L, B, Rw, wide), BF16) for wide in parts],
            dma((Q, 2, 3)), dma((Q, 2, B)),
            dma((2, Q, 2, L)), dma((Q, 2, L)),
            dma((3, 3)), dma((3, B)),
            dma((3, 3, mate)), dma((3, B, T)),
            dma((2, mate, K)), dma((2, T, K)),
            dma((2, K)), dma((2, K)),
            dma((2, K)), dma((2, K)),
            dma((2, mate)), dma((2, T)),
            dma((Q, L)), dma((Q, L)), dma((Q, L)),
            dma((Q, 3)), dma((Q, B)),
        ],
        compiler_params=pltpu.CompilerParams(
            collective_id=0, has_side_effects=True, vmem_limit_bytes=58 * 2**20
        ),
        cost_estimate=pl.CostEstimate(flops=flops, bytes_accessed=2**25, transcendentals=0),
    )(fwd_input, saved_input, out_cotangent, up_weight, down)
    grad_scale = float(rows * n) ** (-0.5)
    anywhere = pl.BlockSpec(memory_space=pl.ANY)
    return pl.pallas_call(
        functools.partial(hand_over, grad_scale),
        out_shape=(
            jax.ShapeDtypeStruct((rows, D), BF16),
            jax.ShapeDtypeStruct((rows, D), BF16),
            jax.ShapeDtypeStruct((Rw, F), F32),
        ),
        in_specs=[anywhere] * 4,
        out_specs=(anywhere,) * 3,
        scratch_shapes=[
            pltpu.VMEM((rows, D), BF16),
            pltpu.VMEM((rows, D), BF16),
            pltpu.VMEM((Rw, F), BF16),
            pltpu.VMEM((Rw, F), F32),
            pltpu.VMEM((Rw, F), F32),
            dma((4, SPLIT)), dma((3, SPLIT)),
        ],
        cost_estimate=pl.CostEstimate(flops=2 * Rw * F, bytes_accessed=14 * Rw * F, transcendentals=0),
    )(layer_out, input_grad, grad, up_grad_sum)


def solution(mesh):
    placed = (
        P("fs", None),
        P("fs", None),
        P("fs", None),
        P("fs", "tp"),
        P("tp", "fs"),
        P("fs", "tp"),
    )
    return jax.shard_map(
        functools.partial(per_device, mesh.shape["fs"], mesh.shape["tp"]),
        mesh=mesh,
        in_specs=placed,
        out_specs=(P("fs", None), P("fs", None), P("fs", "tp")),
        check_vma=False,
    )
```
